256 devices in a mesh: sp: 64 (over z, y, core), tp: 4 (over x).
Axes of the slice: x: 4, y: 4, z: 8, core: 2. Of those that a mesh axis runs over, the one named last changes fastest.
Arguments:
- grad_out: bfloat16 [16384, 2048], P('sp'), may hold values from -16 to 16
- resid: bfloat16 [16384, 2048], P('sp'), may hold values from -6 to 6
- norm_gain: float32 [2048], replicated, may hold values from 0.1 to 1.9
- routes: int32 [16384, 2], P('sp'), may hold values from 0 to 63, all different within a row; in each aligned block of 256 rows (0 to 255, 256 to 511, ...) at most 12 rows name the same one
- route_weights: float32 [16384, 2], P('sp'), may hold values from 0.05 to 1
- gate_weight: bfloat16 [64, 2048, 1536], P('sp', None, 'tp'), may hold values from -0.375 to 0.375
- up_weight: bfloat16 [64, 2048, 1536], P('sp', None, 'tp'), may hold values from -0.375 to 0.375
- down_weight: bfloat16 [64, 1536, 2048], P('sp', 'tp'), may hold values from -0.15625 to 0.15625
- proj_weight: bfloat16 [2048, 512], P(None, 'tp'), may hold values from -0.25 to 0.25
- conv_sum: bfloat16 [16384, 512], P('sp', 'tp'), may hold values from -6 to 6
- conv_gain: float32 [512], P('tp'), may hold values from 0.1 to 1.9
- conv_taps: float32 [31, 512], P(None, 'tp'), may hold values from -1 to 1
- conv_value: bfloat16 [16384, 512], P('sp', 'tp'), may hold values from -6 to 6
- conv_gate: bfloat16 [16384, 512], P('sp', 'tp'), may hold values from -6 to 6
Outputs:
- gate_weight_grad: bfloat16 [64, 2048, 1536], P('sp', None, 'tp')
- up_weight_grad: bfloat16 [64, 2048, 1536], P('sp', None, 'tp')
- down_weight_grad: bfloat16 [64, 1536, 2048], P('sp', 'tp')
- proj_grad: float32 [2048, 512], P('sp', 'tp')
- value_grad: bfloat16 [16384, 512], P('sp', 'tp')
- gate_input_grad: bfloat16 [16384, 512], P('sp', 'tp')
The draws below stay inside these ranges and needn't reach their ends.
Inputs may be any that keep to these rules, and one draw needn't show every extreme that they name: In each aligned block of 256 tokens no expert is named by more than 12 routes, and in some block one expert is named exactly 12 times; a token's two routes name different experts.
All inputs are finite; a program needn't handle non-finite values.
Results may differ from the reference program's by a relative error of at most 0.028.
Values may be sent and summed in bfloat16 or wider, within the bound.
A program may use at most 128 MiB of HBM per device.

```python
import math
import jax
import jax.numpy as jnp
import numpy as np
from jax import lax

D = 2048
F = 1536
CH = 512
CONV_K = 31
TOK_DEV = 256
GROUP = 128
EXPERTS = 64
CAP = 12
TOKENS = 16384
N_SP = 64
N_TP = 4


def raised(result, rng, source, target, blocks, factor):
    owner, partner = [(jnp.arange(result.shape[axis_at]) // (result.shape[axis_at] // blocks)).reshape([-1 if axis == axis_at else 1 for axis in range(result.ndim)]) for axis_at in (source, target)]
    chosen = jax.random.permutation(rng, blocks)[partner]
    strong = (owner == chosen) | (owner == (partner + blocks // 2) % blocks)
    return jnp.where(strong, factor * result, result)


def block_levels(key, extent, pieces, smallest, high):
    loudness = 1.0
    for dim, parts in pieces:
        heights = jax.random.uniform(jax.random.fold_in(jax.random.fold_in(key, 6), dim), (parts,), jnp.float32, smallest / len(pieces), high / len(pieces))
        loudness = loudness * jnp.repeat(jnp.exp(heights), extent[dim] // parts).reshape((-1,) + (1,) * (len(extent) - 1 - dim))
    return loudness


def deal_out(own_key, own, number, rows, number_of, top, reach, skew):
    order = jax.random.permutation(own_key, number_of)
    crowded, ordinary = shares(number_of, rows * top, reach, skew, True), shares(number_of, rows * top, reach, skew, False)
    places = jnp.arange(number_of)

    def named(lengths, rotation):
        used = int((lengths > 0).sum())
        fixed = max(1, used // 4)
        passed = fixed + (places - fixed + rotation * (used - fixed)) % max(1, number_of - fixed)
        return jnp.zeros((number_of,), jnp.int32).at[order[jnp.where(places < fixed, places, passed)]].set(jnp.asarray(lengths, jnp.int32))

    lengths = jnp.where(number % 4 == 0, named(crowded, number // 4), named(ordinary, number - number // 4 - 1))
    mixed = jax.random.permutation(jax.random.fold_in(own, 3), number_of)
    giver, receiver = mixed[0:number_of // 2 * 2:2], mixed[1:number_of // 2 * 2:2]
    room = jnp.minimum(lengths[giver] - 1, reach - lengths[receiver]) // 2
    room = jnp.where((giver == order[0]) | (receiver == order[0]) | (lengths[receiver] == 0), 0, jnp.maximum(room, 0))
    passed = jax.random.randint(jax.random.fold_in(own, 4), (number_of // 2,), 0, 1 << 20) % (room + 1)
    lengths = lengths.at[giver].add(-passed).at[receiver].add(passed)
    items = jnp.searchsorted(jnp.cumsum(lengths), jnp.arange(rows * top), side="right").astype(jnp.int32)
    grid = items.reshape(top, rows).T
    grid = grid[jax.random.permutation(jax.random.fold_in(own, 1), rows)]
    rotation = jax.random.randint(jax.random.fold_in(own, 2), (rows, 1), 0, top)
    return jnp.take_along_axis(grid, (jnp.arange(top)[None, :] + rotation) % top, axis=1)


def shares(amount, total, limit, lean, full):
    portions = [(1 << 20) // math.isqrt(standing ** lean) + 1 for standing in range(1, amount + 1)]
    largest = limit if full else min(limit, max(-(-total // amount), total * portions[0] // sum(portions)))
    least = 1 if total - largest >= amount - 1 else 0
    holding, spare = [largest] + [least] * (amount - 1), total - largest - least * (amount - 1)
    while spare > 0:
        candidates = [i for i in range(1, amount) if holding[i] < largest] or [i for i in range(1, amount) if holding[i] < limit]
        pool, remaining = sum([portions[i] for i in candidates]), spare
        for i in candidates:
            addition = min(limit - holding[i], max(1, remaining * portions[i] // pool), spare)
            holding[i] = holding[i] + addition
            spare = spare - addition
    return np.array(holding)


def gaussian(key, extent, deviation, bound, shards=(), held_as=jnp.bfloat16):
    values = deviation * jax.random.normal(key, extent, jnp.float32)
    if shards:
        values = values * block_levels(key, extent, shards, -0.22, 0.18)
    return jnp.clip(values, -bound, bound).astype(held_as)


def noise_with(rng, dims, deviation, limit, split, heavy, kind=jnp.bfloat16):
    drawn = deviation * jax.random.normal(rng, dims, jnp.float32)
    if split:
        drawn = drawn * block_levels(rng, dims, split, -0.22, 0.18)
    return jnp.clip(raised(drawn, jax.random.fold_in(rng, 3), *heavy), -limit, limit).astype(kind)


def setup_inputs(seed: int = 0) -> dict:
    streams_of = jax.random.split(jax.random.key(seed), 15)
    grad_out = noise_with(streams_of[0], (TOKENS, D), 1.0, 16.0, ((0, 64),), (0, 1, 64, 4.0))
    resid = gaussian(streams_of[1], (TOKENS, D), 1.0, 6.0, ((0, 64),))
    norm_gain = jnp.clip(1.0 + 0.18 * jax.random.normal(streams_of[2], (D,), jnp.float32), 0.1, 1.9)
    routes_keys = jax.random.split(jax.random.fold_in(streams_of[3], 1), TOKENS // TOK_DEV)
    routes_turns = jax.random.permutation(jax.random.fold_in(streams_of[3], 3), TOKENS // TOK_DEV)
    routes = jax.vmap(lambda own, number: deal_out(jax.random.fold_in(streams_of[3], 2), own, number, TOK_DEV, EXPERTS, 2, CAP, 1))(routes_keys, routes_turns).reshape((TOKENS, 2))
    route_weights = jnp.clip(0.05 + 0.95 * jax.random.uniform(streams_of[4], (TOKENS, 2), jnp.float32) ** block_levels(streams_of[4], (TOKENS, 2), ((0, 64),), -0.2, 0.2), 0.05, 1.0)
    gate_weight = gaussian(streams_of[5], (EXPERTS, D, F), (D // 9) ** -0.5, 0.375, ((0, 64), (2, 4)))
    up_weight = gaussian(streams_of[6], (EXPERTS, D, F), (D // 9) ** -0.5, 0.375, ((0, 64), (2, 4)))
    down_weight = gaussian(streams_of[7], (EXPERTS, F, D), F ** -0.5, 0.15625, ((0, 64), (1, 4)))
    proj_weight = gaussian(streams_of[8], (D, CH), CH ** -0.5, 0.25, ((1, 4),))
    conv_sum = gaussian(streams_of[9], (TOKENS, CH), 1.0, 6.0, ((0, 64), (1, 4)))
    conv_gain = jnp.clip(1.0 + 0.18 * jax.random.normal(streams_of[10], (CH,), jnp.float32), 0.1, 1.9)
    conv_taps = gaussian(streams_of[11], (CONV_K, CH), CONV_K ** -0.5, 1.0, ((1, 4),), jnp.float32)
    conv_value = gaussian(streams_of[12], (TOKENS, CH), 1.0, 6.0, ((0, 64), (1, 4)))
    conv_gate = gaussian(streams_of[13], (TOKENS, CH), 1.0, 6.0, ((0, 64), (1, 4)))
    return dict(grad_out=grad_out, resid=resid, norm_gain=norm_gain, routes=routes, route_weights=route_weights, gate_weight=gate_weight, up_weight=up_weight, down_weight=down_weight, proj_weight=proj_weight, conv_sum=conv_sum, conv_gain=conv_gain, conv_taps=conv_taps, conv_value=conv_value, conv_gate=conv_gate)


CLAMP_LIMIT = 7.0
SLOPE_ALPHA = 1.702

def contract_rows(left_side, right_side):
    return lax.dot_general(left_side, right_side, (((0,), (0,)), ((), ())), preferred_element_type=jnp.float32)

def contract_cols(left_side, right_side):
    return lax.dot_general(left_side, right_side, (((1,), (1,)), ((), ())), preferred_element_type=jnp.float32)

def expert_backward(routed_rows, routed_cots, w_gate, w_up, w_down):
    gate_pre = jnp.dot(routed_rows, w_gate, preferred_element_type=jnp.float32)
    up_pre = jnp.dot(routed_rows, w_up, preferred_element_type=jnp.float32)
    gate_clamped = jnp.minimum(gate_pre, CLAMP_LIMIT)
    up_clamped = jnp.clip(up_pre, -CLAMP_LIMIT, CLAMP_LIMIT)
    sigma = jax.nn.sigmoid(SLOPE_ALPHA * gate_clamped)
    gated = gate_clamped * sigma
    act = ((up_clamped + 1.0) * gated).astype(jnp.bfloat16)
    down_grad = contract_rows(act, routed_cots).astype(jnp.bfloat16)
    act_grad = contract_cols(routed_cots, w_down)
    inside = (up_pre > -CLAMP_LIMIT) & (up_pre < CLAMP_LIMIT)
    up_pre_grad = jnp.where(inside, act_grad * gated, 0.0).astype(jnp.bfloat16)
    slope = sigma + SLOPE_ALPHA * gate_clamped * sigma * (1.0 - sigma)
    gate_pre_grad = jnp.where(gate_pre < CLAMP_LIMIT, act_grad * (up_clamped + 1.0) * slope, 0.0).astype(jnp.bfloat16)
    gate_grad = contract_rows(routed_rows, gate_pre_grad).astype(jnp.bfloat16)
    up_grad = contract_rows(routed_rows, up_pre_grad).astype(jnp.bfloat16)
    partial_value = contract_cols(gate_pre_grad, w_gate) + contract_cols(up_pre_grad, w_up)
    return (gate_grad, up_grad, down_grad, partial_value)

def reference(grad_out, resid, norm_gain, routes, route_weights, gate_weight, up_weight, down_weight, proj_weight, conv_sum, conv_gain, conv_taps, conv_value, conv_gate):
    resid_f = resid.astype(jnp.float32)
    inv_rms = lax.rsqrt(lax.optimization_barrier(jnp.mean(resid_f * resid_f, axis=-1, keepdims=True)) + 1e-06)
    normed = (resid_f * inv_rms * norm_gain).astype(jnp.bfloat16)
    scaled = (route_weights[:, :, None] * grad_out.astype(jnp.float32)[:, None, :]).astype(jnp.bfloat16)
    scaled = scaled.reshape(2 * TOKENS, D)
    route_ids = routes.reshape(N_SP, 2 * TOK_DEV)
    one_hot = (route_ids[:, :, None] == jnp.arange(EXPERTS, dtype=jnp.int32)[None, None, :]).astype(jnp.int32)
    slot_rank = lax.optimization_barrier(jnp.sum(jnp.cumsum(one_hot, axis=1) * one_hot, axis=2)) - 1
    slot_index = route_ids * (N_SP * CAP) + jnp.arange(N_SP, dtype=jnp.int32)[:, None] * CAP + slot_rank
    slot_table = jnp.full((EXPERTS * N_SP * CAP,), 2 * TOKENS, jnp.int32)
    slot_table = slot_table.at[slot_index.reshape(-1)].set(jnp.arange(2 * TOKENS, dtype=jnp.int32))
    slot_table = slot_table.reshape(EXPERTS, N_SP * CAP)
    normed_pad = jnp.concatenate([normed, jnp.zeros((1, D), jnp.bfloat16)], axis=0)
    scaled_pad = jnp.concatenate([scaled, jnp.zeros((1, D), jnp.bfloat16)], axis=0)
    block_width = F // N_TP

    def one_expert(route_store, inputs):
        table_row, w_gate, w_up, w_down = inputs
        routed_rows = normed_pad[table_row // 2]
        routed_cots = scaled_pad[table_row]
        gate_parts, up_parts, down_parts = ([], [], [])
        row_total = jnp.zeros((N_SP * CAP, D), jnp.float32)
        for block_number in range(N_TP):
            first_col = block_number * block_width
            gate_grad, up_grad, down_grad, partial_value = expert_backward(routed_rows, routed_cots, w_gate[:, first_col:first_col + block_width], w_up[:, first_col:first_col + block_width], w_down[first_col:first_col + block_width, :])
            gate_parts.append(gate_grad)
            up_parts.append(up_grad)
            down_parts.append(down_grad)
            rounded = lax.optimization_barrier(partial_value.astype(jnp.bfloat16))
            row_total = row_total + rounded.astype(jnp.float32)
        route_store = route_store.at[table_row].set(row_total.astype(jnp.bfloat16))
        return (route_store, (jnp.concatenate(gate_parts, axis=1), jnp.concatenate(up_parts, axis=1), jnp.concatenate(down_parts, axis=0)))
    route_store = jnp.zeros((2 * TOKENS + 1, D), jnp.bfloat16)
    route_store, (gate_weight_grad, up_weight_grad, down_weight_grad) = lax.scan(one_expert, route_store, (slot_table, gate_weight, up_weight, down_weight))
    normed_grad = route_store[:2 * TOKENS].astype(jnp.float32).reshape(TOKENS, 2, D).sum(axis=1).astype(jnp.bfloat16)
    feature_grad = normed_grad.astype(jnp.float32) * norm_gain
    cubed = inv_rms * inv_rms * inv_rms
    resid_grad = (grad_out.astype(jnp.float32) + inv_rms * feature_grad - resid_f * cubed * lax.optimization_barrier(jnp.mean(resid_f * feature_grad, axis=-1, keepdims=True))).astype(jnp.bfloat16)
    summed = conv_sum.astype(jnp.float32).reshape(TOKENS, CH // GROUP, GROUP)
    centre = summed - lax.optimization_barrier(jnp.mean(summed, axis=-1, keepdims=True))
    inv_std = lax.rsqrt(lax.optimization_barrier(jnp.mean(centre * centre, axis=-1, keepdims=True)) + 1e-05)
    grouped = centre * inv_std
    chan_normed = grouped.reshape(TOKENS, CH)
    pre_act = chan_normed * conv_gain
    sigma_conv = jax.nn.sigmoid(pre_act)
    conv_out = (pre_act * sigma_conv).astype(jnp.bfloat16)
    proj_grad = contract_rows(resid_grad, conv_out)
    out_grad = jnp.dot(resid_grad, proj_weight, preferred_element_type=jnp.float32)
    normal_grad = (out_grad * sigma_conv * (1.0 + pre_act * (1.0 - sigma_conv)) * conv_gain).reshape(TOKENS, CH // GROUP, GROUP)
    sum_grad = inv_std * (normal_grad - lax.optimization_barrier(jnp.mean(normal_grad, axis=-1, keepdims=True)) - grouped * lax.optimization_barrier(jnp.mean(normal_grad * grouped, axis=-1, keepdims=True)))
    sum_grad = sum_grad.reshape(TOKENS, CH)
    extended = jnp.concatenate([sum_grad, jnp.zeros((CONV_K - 1, CH), jnp.float32)], axis=0)
    gated_grad = lax.conv_general_dilated(extended[None], conv_taps[::-1][:, None, :], (1,), ((0, 0),), dimension_numbers=('NWC', 'WIO', 'NWC'), feature_group_count=CH, precision=lax.Precision.HIGHEST)[0]
    sigma_gate = jax.nn.sigmoid(conv_gate.astype(jnp.float32))
    value_grad = (gated_grad * sigma_gate).astype(jnp.bfloat16)
    gate_input_grad = (gated_grad * conv_value.astype(jnp.float32) * sigma_gate * (1.0 - sigma_gate)).astype(jnp.bfloat16)
    return (gate_weight_grad, up_weight_grad, down_weight_grad, proj_grad, value_grad, gate_input_grad)
```

```python
import functools

import jax
import jax.numpy as jnp
from jax import lax
from jax.experimental import pallas as pl
from jax.experimental.pallas import tpu as pltpu
from jax.sharding import PartitionSpec as P

CONV_K = 31
GROUP = 128
CAP = 12
CLAMP_LIMIT = 7.0
SLOPE_ALPHA = 1.702
MESH = pl.DeviceIdType.MESH
BF = jnp.bfloat16
F32 = jnp.float32
N_SP = 64
N_TP = 4
NZ = 8
PER_Z = 8
QW = 512
ORDER = (0, 1, 7, 2, 6, 3, 5, 4)
BACK = (4, 3, 5, 2, 6, 1, 7, 0)


def coords():
    sp = lax.axis_index("sp")
    tp = lax.axis_index("tp")
    return sp, tp, lax.rem(tp + 1, N_TP), lax.rem(tp + N_TP - 1, N_TP)


def greet_all(sp, tp, right, left):
    barrier = pltpu.get_barrier_semaphore()

    def hello(i, carry):
        pl.semaphore_signal(
            barrier, inc=1, device_id=(lax.rem(sp + i, N_SP), tp), device_id_type=MESH
        )
        return carry

    lax.fori_loop(1, N_SP, hello, 0)
    pl.semaphore_signal(barrier, inc=1, device_id=(sp, right), device_id_type=MESH)
    pl.semaphore_signal(barrier, inc=1, device_id=(sp, left), device_id_type=MESH)
    pl.semaphore_wait(barrier, N_SP + 1)


def remote(src, dst, send, recv, device):
    return pltpu.make_async_remote_copy(
        src_ref=src, dst_ref=dst, send_sem=send, recv_sem=recv, device_id=device, device_id_type=MESH
    )


def columns(quarter):
    return pl.ds(pl.multiple_of(quarter * QW, QW), QW)


def dispatch_kernel(send_ref, out_ref, a_send, a_recv, x_send, x_recv, r_recv, own_sem):
    sp, tp, right, left = coords()
    z = sp // PER_Z
    mine, from_left, from_right = columns(tp), columns(left), columns(right)
    own = pltpu.make_async_copy(send_ref.at[:, sp], out_ref.at[:, sp, :, mine], own_sem)
    own.start()
    greet_all(sp, tp, right, left)

    def to_peer(peer):
        return remote(
            send_ref.at[:, peer], out_ref.at[:, sp, :, mine], a_send, a_recv.at[z], (peer, tp)
        )

    for dz in ORDER:
        target = lax.rem(z + dz, NZ) * PER_Z

        def send_one(m, carry):
            to_peer(target + lax.rem(sp + m, PER_Z)).start()
            return carry

        lax.fori_loop(1 if dz == 0 else 0, PER_Z, send_one, 0)

    def group(zs, cols, first=0, count=PER_Z):
        return out_ref.at[:, pl.ds(zs * PER_Z + first, count), :, cols]

    def relay(zs):
        half = PER_Z // 2
        remote(group(zs, from_left), group(zs, from_left), x_send, x_recv.at[0, zs], (sp, right)).wait_recv()
        remote(group(zs, from_left, 0, half), group(zs, from_left, 0, half), x_send, r_recv.at[0, zs], (sp, right)).start()
        remote(group(zs, from_right), group(zs, from_right), x_send, x_recv.at[1, zs], (sp, left)).wait_recv()
        remote(group(zs, from_right, half, half), group(zs, from_right, half, half), x_send, r_recv.at[1, zs], (sp, left)).start()

    own.wait()
    previous = None
    for dz in ORDER:
        zs = lax.rem(z + NZ - dz, NZ)
        arrived = group(zs, mine, 0, PER_Z - 1 if dz == 0 else PER_Z)
        remote(arrived, arrived, a_send, a_recv.at[zs], (sp, right)).wait_recv()
        block = group(zs, mine)
        remote(block, block, x_send, x_recv.at[0, zs], (sp, right)).start()
        remote(block, block, x_send, x_recv.at[1, zs], (sp, left)).start()
        if previous is not None:
            relay(previous)
        previous = zs
    relay(previous)
    far = columns(lax.rem(tp + 2, N_TP))
    for dz in ORDER:
        zs = lax.rem(z + NZ - dz, NZ)
        half = PER_Z // 2
        a, b = group(zs, far, 0, half), group(zs, far, half, half)
        remote(a, a, x_send, r_recv.at[0, zs], (sp, right)).wait_recv()
        remote(b, b, x_send, r_recv.at[1, zs], (sp, left)).wait_recv()
        block = group(zs, mine)
        for _ in range(3):
            remote(block, block, x_send, x_recv.at[0, zs], (sp, right)).wait_send()
    sent = send_ref.at[:, pl.ds(0, N_SP - 1)]
    remote(sent, sent, a_send, a_recv.at[0], (sp, right)).wait_send()


def dispatch(send):
    return pl.pallas_call(
        dispatch_kernel,
        out_shape=jax.ShapeDtypeStruct((3, N_SP, 8, N_TP * QW), BF),
        in_specs=[pl.BlockSpec(memory_space=pl.ANY)],
        out_specs=pl.BlockSpec(memory_space=pl.ANY),
        scratch_shapes=[
            pltpu.SemaphoreType.DMA,
            pltpu.SemaphoreType.DMA((NZ,)),
            pltpu.SemaphoreType.DMA,
            pltpu.SemaphoreType.DMA((2, NZ)),
            pltpu.SemaphoreType.DMA((2, NZ)),
            pltpu.SemaphoreType.DMA,
        ],
        compiler_params=pltpu.CompilerParams(collective_id=0, has_side_effects=True),
        name="dispatch",
    )(send)


TILES = 12
HALF = TILES // 2


def return_kernel(
    part_ref, out_ref, opp, near, stage, rows, o_send, o_recv, n_send, n_recv, b_send, b_recv, own_sem
):
    sp, tp, right, left = coords()
    z = sp // PER_Z
    member = lax.rem(sp, PER_Z)
    greet_all(sp, tp, right, left)
    far = columns(lax.rem(tp + 2, N_TP))
    sides = ((0, right, left, 0), (1, left, right, HALF))

    def opposite(side, zs):
        _, ahead, _, first = sides[side]
        return remote(
            part_ref.at[zs, pl.ds(first, HALF), :, far],
            opp.at[side, zs],
            o_send,
            o_recv.at[side, zs],
            (sp, ahead),
        )

    def onward(side, zs):
        return remote(
            stage.at[side, zs], near.at[side, zs], n_send, n_recv.at[side, zs], (sp, sides[side][1])
        )

    def home(zs):
        for side in (0, 1):
            onward(side, zs).wait_recv()
        total = part_ref[zs, :, :, columns(tp)].astype(F32)
        total = total + near[0, zs].astype(F32) + near[1, zs].astype(F32)
        rows[zs] = total.astype(BF)

        def tiles(m):
            return ((m, 0), (PER_Z + m // 2, 1))

        def send_one(m, carry):
            for tile, kind in tiles(m):
                remote(rows.at[zs, tile], out_ref.at[kind, sp], b_send, b_recv, (zs * PER_Z + m, tp)).start()
            return carry

        return send_one, tiles

    order = [lax.rem(z + dz, NZ) for dz in BACK]
    for zs in order:
        for side in (0, 1):
            opposite(side, zs).start()
    for k, zs in enumerate(order + [None]):
        if zs is not None:
            for side in (0, 1):
                _, ahead, _, first = sides[side]
                opposite(side, zs).wait_recv()
                other = HALF - first
                stage[side, zs, pl.ds(first, HALF)] = (
                    part_ref[zs, pl.ds(first, HALF), :, columns(ahead)].astype(F32)
                    + opp[side, zs].astype(F32)
                ).astype(BF)
                stage[side, zs, pl.ds(other, HALF)] = part_ref[zs, pl.ds(other, HALF), :, columns(ahead)]
                onward(side, zs).start()
        if k > 0:
            prev = order[k - 1]
            send_one, tiles = home(prev)
            if BACK[k - 1] != 0:
                lax.fori_loop(0, PER_Z, send_one, 0)
            else:
                lax.fori_loop(1, PER_Z, lambda i, c: send_one(lax.rem(member + i, PER_Z), c), 0)
                for tile, kind in tiles(member):
                    pltpu.make_async_copy(rows.at[prev, tile], out_ref.at[kind, sp], own_sem).start()
    mine = out_ref.at[:, pl.ds(0, 1)]
    pltpu.make_async_copy(mine, mine, own_sem).wait()
    for zs in order:
        for side in (0, 1):
            opposite(side, zs).wait_send()
            onward(side, zs).wait_send()
    rest = out_ref.at[:, pl.ds(0, N_SP - 1)]
    everything = remote(rest, rest, b_send, b_recv, (sp, right))
    everything.wait_recv()
    everything.wait_send()


def send_back(part):
    return pl.pallas_call(
        return_kernel,
        out_shape=jax.ShapeDtypeStruct((2, N_SP, 8, QW), BF),
        in_specs=[pl.BlockSpec(memory_space=pltpu.VMEM)],
        out_specs=pl.BlockSpec(memory_space=pltpu.VMEM),
        scratch_shapes=[
            pltpu.VMEM((2, NZ, HALF, 8, QW), BF),
            pltpu.VMEM((2, NZ, TILES, 8, QW), BF),
            pltpu.VMEM((2, NZ, TILES, 8, QW), BF),
            pltpu.VMEM((NZ, TILES, 8, QW), BF),
            pltpu.SemaphoreType.DMA,
            pltpu.SemaphoreType.DMA((2, NZ)),
            pltpu.SemaphoreType.DMA,
            pltpu.SemaphoreType.DMA((2, NZ)),
            pltpu.SemaphoreType.DMA,
            pltpu.SemaphoreType.DMA,
            pltpu.SemaphoreType.DMA,
        ],
        compiler_params=pltpu.CompilerParams(collective_id=1, has_side_effects=True),
        name="send_back",
    )(part)


def sent_to_all(shard, axis):
    peers = lax.axis_size(axis)
    return lax.all_to_all(
        jnp.broadcast_to(shard[None], (peers, *shard.shape)), axis, 0, 0, tiled=True
    )


def laid_out(parts, dim):
    parts = jnp.moveaxis(parts, 0, dim)
    shape = parts.shape
    return parts.reshape(*shape[:dim], shape[dim] * shape[dim + 1], *shape[dim + 2 :])


def collect(shard, axis, dim):
    parts = sent_to_all(shard, axis)
    return laid_out(parts, dim)


def split_up(shard, dim, peers):
    shape = shard.shape
    parts = shard.reshape(*shape[:dim], peers, shape[dim] // peers, *shape[dim + 1 :])
    return jnp.moveaxis(parts, dim, 0)


def summed_on_arrival(shard, axis, dim):
    parts = split_up(shard, dim, lax.axis_size(axis))
    arrived = lax.all_to_all(parts, axis, split_axis=0, concat_axis=0, tiled=True)
    return arrived.astype(jnp.float32).sum(axis=0)


def passed_along(block, axis, distance):
    devices = range(lax.axis_size(axis))
    route = [(i - distance, i) for i in devices if i - distance in devices]
    return lax.ppermute(block, axis, route)


def contract_rows(left_side, right_side):
    return lax.dot_general(
        left_side, right_side, (((0,), (0,)), ((), ())), preferred_element_type=jnp.float32
    )


def contract_cols(left_side, right_side):
    return lax.dot_general(
        left_side, right_side, (((1,), (1,)), ((), ())), preferred_element_type=jnp.float32
    )


def expert_backward(arrived, w_gate, w_up, w_down):
    width = arrived.shape[-1]
    tall = arrived.reshape(3 * N_SP * 8, width)
    n = N_SP * 8
    with_rows, with_cots = tall[: 2 * n], tall[n:]
    gate_pre = jnp.dot(with_rows, w_gate, preferred_element_type=F32)
    up_pre = jnp.dot(with_rows, w_up, preferred_element_type=F32)
    raw = contract_cols(with_cots, w_down)
    act_grad = jnp.concatenate([raw[n:], jnp.roll(raw[:n], -4, axis=0)], axis=0)
    index = lax.broadcasted_iota(jnp.int32, (2 * n, 1), 0)
    valid = (index < n) | (index % 8 < 4)
    gate_clamped = jnp.minimum(gate_pre, CLAMP_LIMIT)
    up_clamped = jnp.clip(up_pre, -CLAMP_LIMIT, CLAMP_LIMIT)
    sigma = jax.nn.sigmoid(SLOPE_ALPHA * gate_clamped)
    gated = gate_clamped * sigma
    act = jnp.where(valid, (up_clamped + 1.0) * gated, 0.0)
    inside = valid & (up_pre > -CLAMP_LIMIT) & (up_pre < CLAMP_LIMIT)
    up_pre_grad = jnp.where(inside, act_grad * gated, 0.0).astype(BF)
    slope = sigma + SLOPE_ALPHA * gate_clamped * sigma * (1.0 - sigma)
    gate_pre_grad = jnp.where(
        valid & (gate_pre < CLAMP_LIMIT), act_grad * (up_clamped + 1.0) * slope, 0.0
    ).astype(BF)
    act_placed = jnp.concatenate([jnp.roll(act[n:], 4, axis=0), act[:n]], axis=0).astype(BF)
    partial = contract_cols(gate_pre_grad, w_gate) + contract_cols(up_pre_grad, w_up)
    part_a = partial[:n].astype(BF).reshape(NZ, PER_Z, 8, width)
    part_b = partial[n:].reshape(NZ, PER_Z // 2, 2, 8, width)
    packed = jnp.concatenate([part_b[:, :, 0, :4], part_b[:, :, 1, :4]], axis=2).astype(BF)
    back = jnp.concatenate([part_a, packed], axis=1)
    down_grad = contract_rows(act_placed, with_cots).astype(BF)
    gate_grad = contract_rows(with_rows, gate_pre_grad).astype(BF)
    up_grad = contract_rows(with_rows, up_pre_grad).astype(BF)
    return gate_grad, up_grad, down_grad, back


def local(
    grad_out,
    resid,
    norm_gain,
    routes,
    route_weights,
    gate_weight,
    up_weight,
    down_weight,
    proj_weight,
    conv_sum,
    conv_gain,
    conv_taps,
    conv_value,
    conv_gate,
):
    tok_rows, model_width = resid.shape
    tp = lax.axis_index("tp")
    core = lax.axis_index("sp") % 2
    resid_f = resid.astype(F32)
    inv_rms = lax.rsqrt(jnp.mean(resid_f * resid_f, axis=-1, keepdims=True) + 1e-06)
    first_col = tp * QW
    resid_q = lax.dynamic_slice_in_dim(resid, first_col, QW, 1).astype(F32)
    gain_q = lax.dynamic_slice_in_dim(norm_gain, first_col, QW, 0)
    normed_q = (resid_q * inv_rms * gain_q).astype(BF)
    grad_q = lax.dynamic_slice_in_dim(grad_out, first_col, QW, 1)

    experts = lax.broadcasted_iota(jnp.int32, (N_SP, tok_rows), 0)
    hit0 = routes[:, 0][None, :] == experts
    hit1 = routes[:, 1][None, :] == experts
    named = hit0 | hit1
    weight_of = jnp.where(hit0, route_weights[:, 0][None, :], 0.0) + jnp.where(
        hit1, route_weights[:, 1][None, :], 0.0
    )
    earlier = (
        lax.broadcasted_iota(jnp.int32, (tok_rows, tok_rows), 0)
        < lax.broadcasted_iota(jnp.int32, (tok_rows, tok_rows), 1)
    ).astype(BF)
    rank = jnp.dot(named.astype(BF), earlier, preferred_element_type=F32).astype(jnp.int32)
    rank = jnp.where(named, rank, -1)
    lane8 = jnp.arange(8, dtype=jnp.int32)[None, :, None]
    slot_a = rank[:, None, :] == lane8
    slot_b = rank[:, None, :] == 8 + lane8 % 4
    slots = jnp.stack([slot_a, slot_b], axis=0)
    slot_weight = jnp.sum(jnp.where(slots, weight_of[None, :, None, :], 0.0), axis=-1, keepdims=True)
    chosen = slots.astype(BF).reshape(2 * N_SP * 8, tok_rows)
    picked_rows = jnp.dot(chosen, normed_q, preferred_element_type=F32).astype(BF)
    picked_cots = (
        slot_weight.reshape(2 * N_SP * 8, 1) * jnp.dot(chosen, grad_q, preferred_element_type=F32)
    ).astype(BF)
    n = N_SP * 8
    lower = (lax.broadcasted_iota(jnp.int32, (n, 1), 0) % 8) < 4
    mixed = jnp.where(lower, picked_rows[n:], picked_cots[n:])
    send = jnp.concatenate([picked_rows[:n], mixed, picked_cots[:n]], axis=0).reshape(3, N_SP, 8, QW)
    arrived = dispatch(send)
    gate_grad, up_grad, down_grad, back = expert_backward(
        arrived, gate_weight[0], up_weight[0], down_weight[0]
    )
    returned = send_back(back)
    returned = returned.reshape(2 * n, QW)
    owner = lane8 // 4 == core
    back_slots = jnp.stack([slot_a, slot_b & owner], axis=0).astype(BF).reshape(2 * n, tok_rows)
    normed_part_grad = contract_rows(back_slots, returned).astype(BF)
    normed_grad = collect(normed_part_grad, "tp", 1)
    feature_grad = normed_grad.astype(jnp.float32) * norm_gain
    cubed = inv_rms * inv_rms * inv_rms
    resid_grad = (
        grad_out.astype(jnp.float32)
        + inv_rms * feature_grad
        - resid_f * cubed * jnp.mean(resid_f * feature_grad, axis=-1, keepdims=True)
    ).astype(jnp.bfloat16)
    channels = conv_sum.shape[1]
    summed = conv_sum.astype(jnp.float32).reshape(tok_rows, channels // GROUP, GROUP)
    centre = summed - jnp.mean(summed, axis=-1, keepdims=True)
    inv_std = lax.rsqrt(jnp.mean(centre * centre, axis=-1, keepdims=True) + 1e-05)
    grouped = centre * inv_std
    chan_normed = grouped.reshape(tok_rows, channels)
    pre_act = chan_normed * conv_gain
    sigma_conv = jax.nn.sigmoid(pre_act)
    conv_out = (pre_act * sigma_conv).astype(jnp.bfloat16)
    proj_grad = summed_on_arrival(contract_rows(resid_grad, conv_out).astype(jnp.bfloat16), "sp", 0)
    out_grad = jnp.dot(resid_grad, proj_weight, preferred_element_type=jnp.float32)
    normal_grad = (
        out_grad * sigma_conv * (1.0 + pre_act * (1.0 - sigma_conv)) * conv_gain
    ).reshape(tok_rows, channels // GROUP, GROUP)
    sum_grad = inv_std * (
        normal_grad
        - jnp.mean(normal_grad, axis=-1, keepdims=True)
        - grouped * jnp.mean(normal_grad * grouped, axis=-1, keepdims=True)
    )
    sum_grad = sum_grad.reshape(tok_rows, channels)
    following = passed_along(sum_grad[: CONV_K - 1], "sp", -1)
    extended = jnp.concatenate([sum_grad, following], axis=0)
    gated_grad = lax.conv_general_dilated(
        extended[None],
        conv_taps[::-1][:, None, :],
        (1,),
        ((0, 0),),
        dimension_numbers=("NWC", "WIO", "NWC"),
        feature_group_count=channels,
        precision=lax.Precision.HIGHEST,
    )[0]
    sigma_gate = jax.nn.sigmoid(conv_gate.astype(jnp.float32))
    value_grad = (gated_grad * sigma_gate).astype(jnp.bfloat16)
    gate_input_grad = (
        gated_grad * conv_value.astype(jnp.float32) * sigma_gate * (1.0 - sigma_gate)
    ).astype(jnp.bfloat16)
    return (gate_grad[None], up_grad[None], down_grad[None], proj_grad, value_grad, gate_input_grad)


def solution(mesh):
    in_specs = (
        P("sp", None),
        P("sp", None),
        P(),
        P("sp", None),
        P("sp", None),
        P("sp", None, "tp"),
        P("sp", None, "tp"),
        P("sp", "tp", None),
        P(None, "tp"),
        P("sp", "tp"),
        P("tp"),
        P(None, "tp"),
        P("sp", "tp"),
        P("sp", "tp"),
    )
    out_specs = (
        P("sp", None, "tp"),
        P("sp", None, "tp"),
        P("sp", "tp", None),
        P("sp", "tp"),
        P("sp", "tp"),
        P("sp", "tp"),
    )
    return jax.shard_map(local, mesh=mesh, in_specs=in_specs, out_specs=out_specs, check_vma=False)
```

```python
import functools

import jax
import jax.numpy as jnp
from jax import lax
from jax.experimental import pallas as pl
from jax.experimental.pallas import tpu as pltpu
from jax.sharding import PartitionSpec as P

CONV_K = 31
GROUP = 128
CAP = 12
CLAMP_LIMIT = 7.0
SLOPE_ALPHA = 1.702
MESH = pl.DeviceIdType.MESH
BF = jnp.bfloat16
F32 = jnp.float32
N_SP = 64
N_TP = 4
NZ = 8
PER_Z = 8
QW = 512
ORDER = (0, 1, 7, 2, 6, 3, 5, 4)


def coords():
    sp = lax.axis_index("sp")
    tp = lax.axis_index("tp")
    return sp, tp, lax.rem(tp + 1, N_TP), lax.rem(tp + N_TP - 1, N_TP)


def greet_all(sp, tp, right, left):
    barrier = pltpu.get_barrier_semaphore()

    def hello(i, carry):
        pl.semaphore_signal(
            barrier, inc=1, device_id=(lax.rem(sp + i, N_SP), tp), device_id_type=MESH
        )
        return carry

    lax.fori_loop(1, N_SP, hello, 0)
    pl.semaphore_signal(barrier, inc=1, device_id=(sp, right), device_id_type=MESH)
    pl.semaphore_signal(barrier, inc=1, device_id=(sp, left), device_id_type=MESH)
    pl.semaphore_wait(barrier, N_SP + 1)


def remote(src, dst, send, recv, device):
    return pltpu.make_async_remote_copy(
        src_ref=src, dst_ref=dst, send_sem=send, recv_sem=recv, device_id=device, device_id_type=MESH
    )


def columns(quarter):
    return pl.ds(pl.multiple_of(quarter * QW, QW), QW)


TILES = 12
HALF = TILES // 2
FH = 384


def order_of(k):
    odd = lax.rem(k, 2)
    return lax.rem(odd * ((k + 1) // 2) + (1 - odd) * (NZ - k // 2), NZ)


def experts_kernel(
    send_ref, wg_ref, wu_ref, wd_ref, out_ref, gg_out, ug_out, dg_out,
    arr, wg, wu, wd, gpg, upg, act, part, opp, near, stage, rows, gg, ug, dg,
    a_send, a_recv, x_send, x_recv, r_recv, own_sem, w_sem, o_send, o_recv, n_send, n_recv,
    b_send, b_recv, g_sem,
):
    sp, tp, right, left = coords()
    z = sp // PER_Z
    member = lax.rem(sp, PER_Z)
    mine, from_left, from_right = columns(tp), columns(left), columns(right)
    far = columns(lax.rem(tp + 2, N_TP))
    own = pltpu.make_async_copy(send_ref.at[:, sp], arr.at[:, sp, :, mine], own_sem)
    own.start()
    weights = [
        pltpu.make_async_copy(s, d, w_sem.at[i])
        for i, (s, d) in enumerate(((wg_ref, wg), (wu_ref, wu), (wd_ref, wd)))
    ]
    greet_all(sp, tp, right, left)
    for dz in ORDER:
        target = lax.rem(z + dz, NZ) * PER_Z

        def send_one(m, carry):
            peer = target + lax.rem(sp + m, PER_Z)
            remote(send_ref.at[:, peer], arr.at[:, sp, :, mine], a_send, a_recv.at[z], (peer, tp)).start()
            return carry

        lax.fori_loop(1 if dz == 0 else 0, PER_Z, send_one, 0)
    for copy in weights:
        copy.start()

    def group(zs, cols, first=0, count=PER_Z):
        return arr.at[:, pl.ds(zs * PER_Z + first, count), :, cols]

    def arrive(zs, count):
        block = group(zs, mine, 0, count)
        remote(block, block, a_send, a_recv.at[zs], (sp, right)).wait_recv()

    def forward(zs):
        block = group(zs, mine)
        remote(block, block, x_send, x_recv.at[0, zs], (sp, right)).start()
        remote(block, block, x_send, x_recv.at[1, zs], (sp, left)).start()

    half = PER_Z // 2

    def relay(zs):
        remote(group(zs, from_left), group(zs, from_left), x_send, x_recv.at[0, zs], (sp, right)).wait_recv()
        a = group(zs, from_left, 0, half)
        remote(a, a, x_send, r_recv.at[0, zs], (sp, right)).start()
        remote(group(zs, from_right), group(zs, from_right), x_send, x_recv.at[1, zs], (sp, left)).wait_recv()
        b = group(zs, from_right, half, half)
        remote(b, b, x_send, r_recv.at[1, zs], (sp, left)).start()

    sides = ((0, right, 0), (1, left, HALF))

    def opposite(side, zs):
        _, ahead, first = sides[side]
        return remote(
            part.at[zs, pl.ds(first, HALF), :, far], opp.at[side, zs], o_send, o_recv.at[side, zs], (sp, ahead)
        )

    def onward(side, zs):
        return remote(stage.at[side, zs], near.at[side, zs], n_send, n_recv.at[side, zs], (sp, sides[side][1]))

    def compute(zs):
        a, b = group(zs, far, 0, half), group(zs, far, half, half)
        remote(a, a, x_send, r_recv.at[0, zs], (sp, right)).wait_recv()
        remote(b, b, x_send, r_recv.at[1, zs], (sp, left)).wait_recv()
        n = PER_Z * 8
        members = pl.ds(zs * PER_Z, PER_Z)
        with_rows = arr[pl.ds(0, 2), members].reshape(2 * n, N_TP * QW)
        gate_pre = jnp.dot(with_rows, wg[...], preferred_element_type=F32)
        up_pre = jnp.dot(with_rows, wu[...], preferred_element_type=F32)
        with_cots = arr[pl.ds(1, 2), members].reshape(2 * n, N_TP * QW)
        raw = contract_cols(with_cots, wd[...])
        act_grad = jnp.concatenate([raw[n:], pltpu.roll(raw[:n], n - 4, 0)], axis=0)
        index = lax.broadcasted_iota(jnp.int32, (2 * n, FH), 0)
        valid = (index < n) | (lax.rem(index, 8) < 4)
        gate_clamped = jnp.minimum(gate_pre, CLAMP_LIMIT)
        up_clamped = jnp.clip(up_pre, -CLAMP_LIMIT, CLAMP_LIMIT)
        sigma = jax.nn.sigmoid(SLOPE_ALPHA * gate_clamped)
        gated = gate_clamped * sigma
        acted = jnp.where(valid, (up_clamped + 1.0) * gated, 0.0)
        inside = valid & (up_pre > -CLAMP_LIMIT) & (up_pre < CLAMP_LIMIT)
        up_grad = jnp.where(inside, act_grad * gated, 0.0)
        slope = sigma + SLOPE_ALPHA * gate_clamped * sigma * (1.0 - sigma)
        gate_grad = jnp.where(
            valid & (gate_pre < CLAMP_LIMIT), act_grad * (up_clamped + 1.0) * slope, 0.0
        )
        placed = jnp.concatenate([pltpu.roll(acted[n:], 4, 0), acted[:n]], axis=0)
        act[:, members] = placed.reshape(2, PER_Z, 8, FH).astype(BF)
        gpg[:, members] = gate_grad.reshape(2, PER_Z, 8, FH).astype(BF)
        upg[:, members] = up_grad.reshape(2, PER_Z, 8, FH).astype(BF)
        gate_b, up_b = gate_grad.astype(BF), up_grad.astype(BF)
        wide = 512
        for c in range(N_TP * QW // wide):
            cols = slice(c * wide, (c + 1) * wide)
            partial = contract_cols(gate_b, wg[cols]) + contract_cols(up_b, wu[cols])
            part[zs, 0:PER_Z, :, cols] = partial[:n].reshape(PER_Z, 8, wide).astype(BF)
            mixed = partial[n:].reshape(half, 2, 8, wide)
            packed = mixed[:, 0] + pltpu.roll(mixed[:, 1], 4, 1)
            part[zs, PER_Z:TILES, :, cols] = packed.astype(BF)
        for side in (0, 1):
            opposite(side, zs).start()

    def pass_on(zs):
        for side in (0, 1):
            _, ahead, first = sides[side]
            opposite(side, zs).wait_recv()
            other = HALF - first
            stage[side, zs, pl.ds(first, HALF)] = (
                part[zs, pl.ds(first, HALF), :, columns(ahead)].astype(F32) + opp[side, zs].astype(F32)
            ).astype(BF)
            stage[side, zs, pl.ds(other, HALF)] = part[zs, pl.ds(other, HALF), :, columns(ahead)]
            onward(side, zs).start()

    def home(zs, at_home):
        for side in (0, 1):
            onward(side, zs).wait_recv()
        total = part[zs, :, :, mine].astype(F32)
        total = total + near[0, zs].astype(F32) + near[1, zs].astype(F32)
        rows[zs] = total.astype(BF)

        def send_one(i, carry):
            m = lax.rem(member + i, PER_Z)
            for tile, kind in ((m, 0), (PER_Z + m // 2, 1)):
                remote(rows.at[zs, tile], out_ref.at[kind, sp], b_send, b_recv, (zs * PER_Z + m, tp)).start()
            return carry

        if at_home:
            for tile, kind in ((member, 0), (PER_Z + member // 2, 1)):
                pltpu.make_async_copy(rows.at[zs, tile], out_ref.at[kind, sp], g_sem).start()
        lax.fori_loop(1 if at_home else 0, PER_Z, send_one, 0)

    def source(k):
        return lax.rem(z + NZ - order_of(k), NZ)

    def step(k, carry):
        @pl.when(k == 0)
        def _():
            own.wait()
            arrive(z, PER_Z - 1)
            forward(z)

        @pl.when((k > 0) & (k < NZ))
        def _():
            zs = source(k)
            arrive(zs, PER_Z)
            forward(zs)

        @pl.when((k >= 1) & (k <= NZ))
        def _():
            relay(source(k - 1))

        @pl.when(k == 2)
        def _():
            for copy in weights:
                copy.wait()

        @pl.when((k >= 2) & (k <= NZ + 1))
        def _():
            compute(source(k - 2))

        @pl.when((k >= 3) & (k <= NZ + 2))
        def _():
            pass_on(source(k - 3))

        @pl.when(k == 4)
        def _():
            home(z, True)

        @pl.when(k >= 5)
        def _():
            home(source(k - 4), False)

        return carry

    lax.fori_loop(0, NZ + 4, step, 0)

    n = N_SP * 8
    wide = 256
    outs = [pltpu.make_async_copy(s, d, own_sem) for s, d in ((gg, gg_out), (ug, ug_out), (dg, dg_out))]

    def weight_grads(c, carry):
        cols = pl.ds(pl.multiple_of(c * wide, wide), wide)
        lhs = arr[pl.ds(0, 2), :, :, cols].reshape(2 * n, wide)
        gg[cols] = contract_rows(lhs, gpg[...].reshape(2 * n, FH)).astype(BF)
        ug[cols] = contract_rows(lhs, upg[...].reshape(2 * n, FH)).astype(BF)
        rhs = arr[pl.ds(1, 2), :, :, cols].reshape(2 * n, wide)
        dg[:, cols] = contract_rows(act[...].reshape(2 * n, FH), rhs).astype(BF)
        return carry

    lax.fori_loop(0, N_TP * QW // wide, weight_grads, 0)
    for copy in outs:
        copy.start()

    two = out_ref.at[:, pl.ds(0, 1)]
    pltpu.make_async_copy(two, two, g_sem).wait()

    def drain(zs, carry):
        block = group(zs, mine)
        for _ in range(3):
            remote(block, block, x_send, x_recv.at[0, zs], (sp, right)).wait_send()
        for side in (0, 1):
            opposite(side, zs).wait_send()
            onward(side, zs).wait_send()
        return carry

    lax.fori_loop(0, NZ, drain, 0)
    sent = send_ref.at[:, pl.ds(0, N_SP - 1)]
    remote(sent, sent, a_send, a_recv.at[0], (sp, right)).wait_send()
    for copy in outs:
        copy.wait()
    rest = out_ref.at[:, pl.ds(0, N_SP - 1)]
    everything = remote(rest, rest, b_send, b_recv, (sp, right))
    everything.wait_recv()
    everything.wait_send()


def run_experts(send, w_gate, w_up, w_down):
    width = N_TP * QW
    any_spec = pl.BlockSpec(memory_space=pl.ANY)
    return pl.pallas_call(
        experts_kernel,
        out_shape=(
            jax.ShapeDtypeStruct((2, N_SP, 8, QW), BF),
            jax.ShapeDtypeStruct((width, FH), BF),
            jax.ShapeDtypeStruct((width, FH), BF),
            jax.ShapeDtypeStruct((FH, width), BF),
        ),
        in_specs=[any_spec] * 4,
        out_specs=(pl.BlockSpec(memory_space=pltpu.VMEM), any_spec, any_spec, any_spec),
        scratch_shapes=[
            pltpu.VMEM((3, N_SP, 8, width), BF),
            pltpu.VMEM((width, FH), BF),
            pltpu.VMEM((width, FH), BF),
            pltpu.VMEM((FH, width), BF),
            pltpu.VMEM((2, N_SP, 8, FH), BF),
            pltpu.VMEM((2, N_SP, 8, FH), BF),
            pltpu.VMEM((2, N_SP, 8, FH), BF),
            pltpu.VMEM((NZ, TILES, 8, width), BF),
            pltpu.VMEM((2, NZ, HALF, 8, QW), BF),
            pltpu.VMEM((2, NZ, TILES, 8, QW), BF),
            pltpu.VMEM((2, NZ, TILES, 8, QW), BF),
            pltpu.VMEM((NZ, TILES, 8, QW), BF),
            pltpu.VMEM((width, FH), BF),
            pltpu.VMEM((width, FH), BF),
            pltpu.VMEM((FH, width), BF),
            pltpu.SemaphoreType.DMA,
            pltpu.SemaphoreType.DMA((NZ,)),
            pltpu.SemaphoreType.DMA,
            pltpu.SemaphoreType.DMA((2, NZ)),
            pltpu.SemaphoreType.DMA((2, NZ)),
            pltpu.SemaphoreType.DMA,
            pltpu.SemaphoreType.DMA((3,)),
            pltpu.SemaphoreType.DMA,
            pltpu.SemaphoreType.DMA((2, NZ)),
            pltpu.SemaphoreType.DMA,
            pltpu.SemaphoreType.DMA((2, NZ)),
            pltpu.SemaphoreType.DMA,
            pltpu.SemaphoreType.DMA,
            pltpu.SemaphoreType.DMA,
        ],
        compiler_params=pltpu.CompilerParams(collective_id=0, has_side_effects=True),
        name="experts",
    )(send, w_gate, w_up, w_down)


def sent_to_all(shard, axis):
    peers = lax.axis_size(axis)
    return lax.all_to_all(
        jnp.broadcast_to(shard[None], (peers, *shard.shape)), axis, 0, 0, tiled=True
    )


def laid_out(parts, dim):
    parts = jnp.moveaxis(parts, 0, dim)
    shape = parts.shape
    return parts.reshape(*shape[:dim], shape[dim] * shape[dim + 1], *shape[dim + 2 :])


def collect(shard, axis, dim):
    parts = sent_to_all(shard, axis)
    return laid_out(parts, dim)


def split_up(shard, dim, peers):
    shape = shard.shape
    parts = shard.reshape(*shape[:dim], peers, shape[dim] // peers, *shape[dim + 1 :])
    return jnp.moveaxis(parts, dim, 0)


def summed_on_arrival(shard, axis, dim):
    parts = split_up(shard, dim, lax.axis_size(axis))
    arrived = lax.all_to_all(parts, axis, split_axis=0, concat_axis=0, tiled=True)
    return arrived.astype(jnp.float32).sum(axis=0)


def passed_along(block, axis, distance):
    devices = range(lax.axis_size(axis))
    route = [(i - distance, i) for i in devices if i - distance in devices]
    return lax.ppermute(block, axis, route)


def contract_rows(left_side, right_side):
    return lax.dot_general(
        left_side, right_side, (((0,), (0,)), ((), ())), preferred_element_type=jnp.float32
    )


def contract_cols(left_side, right_side):
    return lax.dot_general(
        left_side, right_side, (((1,), (1,)), ((), ())), preferred_element_type=jnp.float32
    )


def local(
    grad_out,
    resid,
    norm_gain,
    routes,
    route_weights,
    gate_weight,
    up_weight,
    down_weight,
    proj_weight,
    conv_sum,
    conv_gain,
    conv_taps,
    conv_value,
    conv_gate,
):
    tok_rows, model_width = resid.shape
    tp = lax.axis_index("tp")
    core = lax.axis_index("sp") % 2
    resid_f = resid.astype(F32)
    inv_rms = lax.rsqrt(jnp.mean(resid_f * resid_f, axis=-1, keepdims=True) + 1e-06)
    first_col = tp * QW
    resid_q = lax.dynamic_slice_in_dim(resid, first_col, QW, 1).astype(F32)
    gain_q = lax.dynamic_slice_in_dim(norm_gain, first_col, QW, 0)
    normed_q = (resid_q * inv_rms * gain_q).astype(BF)
    grad_q = lax.dynamic_slice_in_dim(grad_out, first_col, QW, 1)

    experts = lax.broadcasted_iota(jnp.int32, (N_SP, tok_rows), 0)
    hit0 = routes[:, 0][None, :] == experts
    hit1 = routes[:, 1][None, :] == experts
    named = hit0 | hit1
    weight_of = jnp.where(hit0, route_weights[:, 0][None, :], 0.0) + jnp.where(
        hit1, route_weights[:, 1][None, :], 0.0
    )
    earlier = (
        lax.broadcasted_iota(jnp.int32, (tok_rows, tok_rows), 0)
        < lax.broadcasted_iota(jnp.int32, (tok_rows, tok_rows), 1)
    ).astype(BF)
    rank = jnp.dot(named.astype(BF), earlier, preferred_element_type=F32).astype(jnp.int32)
    rank = jnp.where(named, rank, -1)
    lane8 = jnp.arange(8, dtype=jnp.int32)[None, :, None]
    slot_a = rank[:, None, :] == lane8
    slot_b = rank[:, None, :] == 8 + lane8 % 4
    slots = jnp.stack([slot_a, slot_b], axis=0)
    slot_weight = jnp.sum(jnp.where(slots, weight_of[None, :, None, :], 0.0), axis=-1, keepdims=True)
    chosen = slots.astype(BF).reshape(2 * N_SP * 8, tok_rows)
    picked_rows = jnp.dot(chosen, normed_q, preferred_element_type=F32).astype(BF)
    picked_cots = (
        slot_weight.reshape(2 * N_SP * 8, 1) * jnp.dot(chosen, grad_q, preferred_element_type=F32)
    ).astype(BF)
    n = N_SP * 8
    lower = (lax.broadcasted_iota(jnp.int32, (n, 1), 0) % 8) < 4
    mixed = jnp.where(lower, picked_rows[n:], picked_cots[n:])
    send = jnp.concatenate([picked_rows[:n], mixed, picked_cots[:n]], axis=0).reshape(3, N_SP, 8, QW)
    returned, gate_grad, up_grad, down_grad = run_experts(
        send, gate_weight[0], up_weight[0], down_weight[0]
    )
    returned = returned.reshape(2 * n, QW)
    owner = lane8 // 4 == core
    back_slots = jnp.stack([slot_a, slot_b & owner], axis=0).astype(BF).reshape(2 * n, tok_rows)
    normed_part_grad = contract_rows(back_slots, returned).astype(BF)
    normed_grad = collect(normed_part_grad, "tp", 1)
    feature_grad = normed_grad.astype(jnp.float32) * norm_gain
    cubed = inv_rms * inv_rms * inv_rms
    resid_grad = (
        grad_out.astype(jnp.float32)
        + inv_rms * feature_grad
        - resid_f * cubed * jnp.mean(resid_f * feature_grad, axis=-1, keepdims=True)
    ).astype(jnp.bfloat16)
    channels = conv_sum.shape[1]
    summed = conv_sum.astype(jnp.float32).reshape(tok_rows, channels // GROUP, GROUP)
    centre = summed - jnp.mean(summed, axis=-1, keepdims=True)
    inv_std = lax.rsqrt(jnp.mean(centre * centre, axis=-1, keepdims=True) + 1e-05)
    grouped = centre * inv_std
    chan_normed = grouped.reshape(tok_rows, channels)
    pre_act = chan_normed * conv_gain
    sigma_conv = jax.nn.sigmoid(pre_act)
    conv_out = (pre_act * sigma_conv).astype(jnp.bfloat16)
    proj_grad = summed_on_arrival(contract_rows(resid_grad, conv_out).astype(jnp.bfloat16), "sp", 0)
    out_grad = jnp.dot(resid_grad, proj_weight, preferred_element_type=jnp.float32)
    normal_grad = (
        out_grad * sigma_conv * (1.0 + pre_act * (1.0 - sigma_conv)) * conv_gain
    ).reshape(tok_rows, channels // GROUP, GROUP)
    sum_grad = inv_std * (
        normal_grad
        - jnp.mean(normal_grad, axis=-1, keepdims=True)
        - grouped * jnp.mean(normal_grad * grouped, axis=-1, keepdims=True)
    )
    sum_grad = sum_grad.reshape(tok_rows, channels)
    following = passed_along(sum_grad[: CONV_K - 1], "sp", -1)
    extended = jnp.concatenate([sum_grad, following], axis=0)
    gated_grad = lax.conv_general_dilated(
        extended[None],
        conv_taps[::-1][:, None, :],
        (1,),
        ((0, 0),),
        dimension_numbers=("NWC", "WIO", "NWC"),
        feature_group_count=channels,
        precision=lax.Precision.HIGHEST,
    )[0]
    sigma_gate = jax.nn.sigmoid(conv_gate.astype(jnp.float32))
    value_grad = (gated_grad * sigma_gate).astype(jnp.bfloat16)
    gate_input_grad = (
        gated_grad * conv_value.astype(jnp.float32) * sigma_gate * (1.0 - sigma_gate)
    ).astype(jnp.bfloat16)
    return (gate_grad[None], up_grad[None], down_grad[None], proj_grad, value_grad, gate_input_grad)


def solution(mesh):
    in_specs = (
        P("sp", None),
        P("sp", None),
        P(),
        P("sp", None),
        P("sp", None),
        P("sp", None, "tp"),
        P("sp", None, "tp"),
        P("sp", "tp", None),
        P(None, "tp"),
        P("sp", "tp"),
        P("tp"),
        P(None, "tp"),
        P("sp", "tp"),
        P("sp", "tp"),
    )
    out_specs = (
        P("sp", None, "tp"),
        P("sp", None, "tp"),
        P("sp", "tp", None),
        P("sp", "tp"),
        P("sp", "tp"),
        P("sp", "tp"),
    )
    return jax.shard_map(local, mesh=mesh, in_specs=in_specs, out_specs=out_specs, check_vma=False)
```

```python
import jax
import jax.numpy as jnp
from jax import lax
from jax.experimental import pallas as pl
from jax.experimental.pallas import tpu as pltpu
from jax.sharding import PartitionSpec as P

CONV_K = 31
GROUP = 128
CAP = 12
CLAMP_LIMIT = 7.0
SLOPE_ALPHA = 1.702
MESH = pl.DeviceIdType.MESH
BF = jnp.bfloat16
F32 = jnp.float32
N_SP = 64
N_TP = 4
NZ = 8
PER_Z = 8
QW = 512
GROUPS = (0, 2, 6, 3, 5, 4, 1, 7)
NARROW = 5
WIDE = (0, 6, 7)


def coords():
    sp = lax.axis_index("sp")
    tp = lax.axis_index("tp")
    return sp, tp, lax.rem(tp + 1, N_TP), lax.rem(tp + N_TP - 1, N_TP)


def greet_all(sp, tp, right, left):
    barrier = pltpu.get_barrier_semaphore()

    def hello(i, carry):
        pl.semaphore_signal(
            barrier, inc=1, device_id=(lax.rem(sp + i, N_SP), tp), device_id_type=MESH
        )
        return carry

    lax.fori_loop(1, N_SP, hello, 0)
    pl.semaphore_signal(barrier, inc=1, device_id=(sp, right), device_id_type=MESH)
    pl.semaphore_signal(barrier, inc=1, device_id=(sp, left), device_id_type=MESH)
    return barrier


def remote(src, dst, send, recv, device):
    return pltpu.make_async_remote_copy(
        src_ref=src, dst_ref=dst, send_sem=send, recv_sem=recv, device_id=device, device_id_type=MESH
    )


def columns(quarter):
    return pl.ds(pl.multiple_of(quarter * QW, QW), QW)


TILES = 12
HALF = TILES // 2
FH = 384


def distance(k):
    total = 0
    for i, dz in enumerate(GROUPS):
        total = total + jnp.where(k == i, dz, 0)
    return total


TOK = 256
RB = 16
HALO = 32
CB = 128


def conv_before(csum_ref, cgain_ref, chan, inv_std, dact, conv_out):
    summed = csum_ref[...].astype(F32)
    centre = summed - jnp.mean(summed, axis=-1, keepdims=True)
    scale = lax.rsqrt(jnp.mean(centre * centre, axis=-1, keepdims=True) + 1e-05)
    grouped = centre * scale
    pre_act = grouped * cgain_ref[...]
    sigma = jax.nn.sigmoid(pre_act)
    chan[...] = grouped
    inv_std[...] = scale
    conv_out[...] = (pre_act * sigma).astype(BF)
    dact[...] = sigma * (1.0 + pre_act * (1.0 - sigma)) * cgain_ref[...]


def choose(z, core, routes_ref, weights_ref, chosen, back, slot_weight):
    named, weight = [], []
    for dz in GROUPS:
        expert = lax.rem(z + dz, NZ) * PER_Z + lax.broadcasted_iota(jnp.int32, (PER_Z, TOK), 0)
        hits = [routes_ref[k : k + 1] == expert for k in (0, 1)]
        named.append(jnp.where(hits[0] | hits[1], 1.0, 0.0))
        weight.append(
            jnp.where(hits[0], weights_ref[0:1], 0.0) + jnp.where(hits[1], weights_ref[1:2], 0.0)
        )
    earlier = lax.broadcasted_iota(jnp.int32, (TOK, TOK), 0) < lax.broadcasted_iota(jnp.int32, (TOK, TOK), 1)
    earlier = jnp.where(earlier, 1.0, 0.0).astype(BF)
    named = jnp.concatenate(named, axis=0)
    rank = jnp.dot(named.astype(BF), earlier, preferred_element_type=F32)
    rank = jnp.where(named > 0.5, rank, -1.0)
    lane = lax.broadcasted_iota(jnp.int32, (PER_Z, 8, TOK), 1)
    slot_a = lane.astype(F32)
    slot_b = (8 + lax.rem(lane, 4)).astype(F32)
    owned = lane // 4 == core
    n = PER_Z * 8
    for i in range(NZ):
        ranks = rank[i * PER_Z : (i + 1) * PER_Z].reshape(PER_Z, 1, TOK)
        weights = weight[i].reshape(PER_Z, 1, TOK)
        for kind, slot in enumerate((slot_a, slot_b)):
            hit = ranks == slot
            rows = slice(kind * n, (kind + 1) * n)
            chosen[i, rows] = jnp.where(hit, 1.0, 0.0).reshape(n, TOK).astype(BF)
            kept = hit & owned if kind else hit
            back[kind, i] = jnp.where(kept, 1.0, 0.0).reshape(n, TOK).astype(BF)
            slot_weight[i, rows] = jnp.sum(jnp.where(hit, weights, 0.0), axis=-1, keepdims=True).reshape(n, 1)


def experts_kernel(
    routes_ref, weights_ref, wg_ref, wu_ref, wd_ref, resid_ref, grad_ref, proj_ref, gain_ref,
    csum_ref, cgain_ref, taps_ref, cval_ref, cgate_ref,
    gg, ug, dg, proj_out, value_out, gatein_out,
    ret, arr, wg, wu, wd, gpg, upg, act, part, opp, near, stage, rows,
    resid, grad, normed, chosen, back, slot_weight, wide_send, narrow_send,
    proj_w, inv, chan, inv_std, dact, conv_out, normed_grad, resid_grad,
    pbuf, pswap, pstage, precv, ext,
    t_sem, s_send, s_recv, s_relay, p_send, p_recv, q_send, q_recv, h_send, h_recv,
    w_send, a_send, a_recv, x_send, x_recv, r_recv, w_sem, o_send, o_recv, n_send, n_recv,
    b_send, b_recv,
):
    sp, tp, right, left = coords()
    z = sp // PER_Z
    member = lax.rem(sp, PER_Z)
    core = lax.rem(sp, 2)
    mine, from_left, from_right = columns(tp), columns(left), columns(right)
    far = columns(lax.rem(tp + 2, N_TP))
    loads = [
        pltpu.make_async_copy(s, d, t_sem.at[i])
        for i, (s, d) in enumerate(((resid_ref, resid), (grad_ref, grad), (proj_ref, proj_w)))
    ]
    weights = [
        pltpu.make_async_copy(s, d, w_sem.at[i])
        for i, (s, d) in enumerate(((wg_ref, wg), (wu_ref, wu), (wd_ref, wd)))
    ]
    for copy in loads + weights:
        copy.start()
    barrier = greet_all(sp, tp, right, left)
    choose(z, core, routes_ref, weights_ref, chosen, back, slot_weight)
    loads[0].wait()

    def norm_block(r, carry):
        block = pl.ds(pl.multiple_of(r * RB, RB), RB)
        x = resid[block].astype(F32)
        scale = lax.rsqrt(jnp.mean(x * x, axis=-1, keepdims=True) + 1e-06)
        inv[block] = scale
        normed[block] = (x * scale * gain_ref[...]).astype(BF)
        return carry

    lax.fori_loop(0, TOK // RB, norm_block, 0)
    loads[1].wait()
    lower = lax.rem(lax.broadcasted_iota(jnp.int32, (PER_Z * 8, QW), 0), 8) < 4

    def pick(i, cols, target, into):
        n = PER_Z * 8
        picked = jnp.dot(chosen[i], normed[:, cols], preferred_element_type=F32)
        cots = slot_weight[i] * jnp.dot(chosen[i], grad[:, cols], preferred_element_type=F32)
        mixed = jnp.where(lower, picked[n:], cots[n:])
        for kind, value in enumerate((picked[:n], mixed, cots[:n])):
            target[:, kind, :, into] = value.reshape(PER_Z, 8, QW).astype(BF)

    def build(i):
        if i in WIDE:
            for c in range(N_TP):
                cols = slice(c * QW, (c + 1) * QW)
                pick(i, cols, wide_send.at[pl.ds(WIDE.index(i) * PER_Z, PER_Z)], cols)
        else:
            pick(i, mine, narrow_send.at[pl.ds((i - 1) * PER_Z, PER_Z)], slice(0, QW))

    def dispatch(i):
        target = lax.rem(z + GROUPS[i], NZ) * PER_Z

        def send_one(m, carry):
            other = lax.rem(sp + m, PER_Z)
            if i in WIDE:
                copy = remote(
                    wide_send.at[WIDE.index(i) * PER_Z + other], arr.at[:, sp], w_send, a_recv.at[z], (target + other, tp)
                )
            else:
                copy = remote(
                    narrow_send.at[(i - 1) * PER_Z + other], arr.at[:, sp, :, mine], a_send, a_recv.at[z], (target + other, tp)
                )
            copy.start()
            return carry

        lax.fori_loop(1 if i == 0 else 0, PER_Z, send_one, 0)

    for i in range(NZ):
        build(i)
        if i == 0:
            arr[:, sp] = wide_send[member]
            pl.semaphore_wait(barrier, N_SP + 1)
        else:
            dispatch(i - 1)
    dispatch(NZ - 1)
    conv_before(csum_ref, cgain_ref, chan, inv_std, dact, conv_out)

    def group(zs, cols, first=0, count=PER_Z):
        return arr.at[:, pl.ds(zs * PER_Z + first, count), :, cols]

    def arrive(zs, cols, count):
        block = group(zs, cols, 0, count)
        remote(block, block, a_send, a_recv.at[zs], (sp, right)).wait_recv()

    everything = pl.ds(0, N_TP * QW)

    def forward(zs):
        block = group(zs, mine)
        remote(block, block, x_send, x_recv.at[0, zs], (sp, right)).start()
        remote(block, block, x_send, x_recv.at[1, zs], (sp, left)).start()

    half = PER_Z // 2

    def relay(zs):
        remote(group(zs, from_left), group(zs, from_left), x_send, x_recv.at[0, zs], (sp, right)).wait_recv()
        a = group(zs, from_left, 0, half)
        remote(a, a, x_send, r_recv.at[0, zs], (sp, right)).start()
        remote(group(zs, from_right), group(zs, from_right), x_send, x_recv.at[1, zs], (sp, left)).wait_recv()
        b = group(zs, from_right, half, half)
        remote(b, b, x_send, r_recv.at[1, zs], (sp, left)).start()

    sides = ((0, right, 0), (1, left, HALF))

    def opposite(side, zs):
        _, ahead, first = sides[side]
        return remote(
            part.at[zs, pl.ds(first, HALF), :, far], opp.at[side, zs], o_send, o_recv.at[side, zs], (sp, ahead)
        )

    def onward(side, zs):
        return remote(stage.at[side, zs], near.at[side, zs], n_send, n_recv.at[side, zs], (sp, sides[side][1]))

    def relayed(zs):
        a, b = group(zs, far, 0, half), group(zs, far, half, half)
        remote(a, a, x_send, r_recv.at[0, zs], (sp, right)).wait_recv()
        remote(b, b, x_send, r_recv.at[1, zs], (sp, left)).wait_recv()

    def compute(zs):
        n = PER_Z * 8
        members = pl.ds(zs * PER_Z, PER_Z)
        with_rows = arr[pl.ds(0, 2), members].reshape(2 * n, N_TP * QW)
        gate_pre = jnp.dot(with_rows, wg[...], preferred_element_type=F32)
        up_pre = jnp.dot(with_rows, wu[...], preferred_element_type=F32)
        with_cots = arr[pl.ds(1, 2), members].reshape(2 * n, N_TP * QW)
        raw = contract_cols(with_cots, wd[...])
        act_grad = jnp.concatenate([raw[n:], pltpu.roll(raw[:n], n - 4, 0)], axis=0)
        index = lax.broadcasted_iota(jnp.int32, (2 * n, FH), 0)
        valid = (index < n) | (lax.rem(index, 8) < 4)
        gate_clamped = jnp.minimum(gate_pre, CLAMP_LIMIT)
        up_clamped = jnp.clip(up_pre, -CLAMP_LIMIT, CLAMP_LIMIT)
        sigma = jax.nn.sigmoid(SLOPE_ALPHA * gate_clamped)
        gated = gate_clamped * sigma
        acted = jnp.where(valid, (up_clamped + 1.0) * gated, 0.0)
        inside = valid & (up_pre > -CLAMP_LIMIT) & (up_pre < CLAMP_LIMIT)
        up_grad = jnp.where(inside, act_grad * gated, 0.0)
        slope = sigma + SLOPE_ALPHA * gate_clamped * sigma * (1.0 - sigma)
        gate_grad = jnp.where(
            valid & (gate_pre < CLAMP_LIMIT), act_grad * (up_clamped + 1.0) * slope, 0.0
        )
        placed = jnp.concatenate([pltpu.roll(acted[n:], 4, 0), acted[:n]], axis=0)
        act[:, members] = placed.reshape(2, PER_Z, 8, FH).astype(BF)
        gpg[:, members] = gate_grad.reshape(2, PER_Z, 8, FH).astype(BF)
        upg[:, members] = up_grad.reshape(2, PER_Z, 8, FH).astype(BF)
        gate_b, up_b = gate_grad.astype(BF), up_grad.astype(BF)
        wide = 512
        for c in range(N_TP * QW // wide):
            cols = slice(c * wide, (c + 1) * wide)
            partial = contract_cols(gate_b, wg[cols]) + contract_cols(up_b, wu[cols])
            part[zs, 0:PER_Z, :, cols] = partial[:n].reshape(PER_Z, 8, wide).astype(BF)
            mixed = partial[n:].reshape(half, 2, 8, wide)
            packed = mixed[:, 0] + pltpu.roll(mixed[:, 1], 4, 1)
            part[zs, PER_Z:TILES, :, cols] = packed.astype(BF)
        for side in (0, 1):
            opposite(side, zs).start()

    def pass_on(zs):
        for side in (0, 1):
            _, ahead, first = sides[side]
            opposite(side, zs).wait_recv()
            other = HALF - first
            stage[side, zs, pl.ds(first, HALF)] = (
                part[zs, pl.ds(first, HALF), :, columns(ahead)].astype(F32) + opp[side, zs].astype(F32)
            ).astype(BF)
            stage[side, zs, pl.ds(other, HALF)] = part[zs, pl.ds(other, HALF), :, columns(ahead)]
            onward(side, zs).start()

    def home(k, zs, at_home):
        for side in (0, 1):
            onward(side, zs).wait_recv()
        total = part[zs, :, :, mine].astype(F32)
        total = total + near[0, zs].astype(F32) + near[1, zs].astype(F32)
        rows[zs] = total.astype(BF)

        def send_one(i, carry):
            m = lax.rem(member + i, PER_Z)
            for tile, kind in ((m, 0), (PER_Z + m // 2, 1)):
                remote(rows.at[zs, tile], ret.at[kind, k * PER_Z + member], b_send, b_recv, (zs * PER_Z + m, tp)).start()
            return carry

        if at_home:
            for tile, kind in ((member, 0), (PER_Z + member // 2, 1)):
                ret[kind, k * PER_Z + member] = rows[zs, tile]
        lax.fori_loop(1 if at_home else 0, PER_Z, send_one, 0)

    def source(k):
        return lax.rem(z + NZ - distance(k), NZ)

    n = N_SP * 8
    wide = 256

    def weight_grads(c, carry):
        cols = pl.ds(pl.multiple_of(c * wide, wide), wide)
        lhs = arr[pl.ds(0, 2), :, :, cols].reshape(2 * n, wide)
        gg[cols] = contract_rows(lhs, gpg[...].reshape(2 * n, FH)).astype(BF)
        ug[cols] = contract_rows(lhs, upg[...].reshape(2 * n, FH)).astype(BF)
        rhs = arr[pl.ds(1, 2), :, :, cols].reshape(2 * n, wide)
        dg[:, cols] = contract_rows(act[...].reshape(2 * n, FH), rhs).astype(BF)
        return carry

    arrive(z, everything, PER_Z - 1)
    for copy in weights:
        copy.wait()
    compute(z)

    def step(k, carry):
        @pl.when(k < NARROW)
        def _():
            zs = source(k + 1)
            arrive(zs, mine, PER_Z)
            forward(zs)

        @pl.when((k >= 1) & (k <= NARROW))
        def _():
            relay(source(k))

        @pl.when((k >= 2) & (k < NARROW + 2))
        def _():
            relayed(source(k - 1))

        @pl.when((k >= NARROW + 2) & (k <= NZ))
        def _():
            arrive(source(k - 1), everything, PER_Z)

        @pl.when((k >= 2) & (k <= NZ))
        def _():
            compute(source(k - 1))

        first = jnp.where(k <= NZ, 0, (k - NZ - 1) * 3)
        stop = jnp.where(k <= NZ, 0, jnp.minimum(first + 3, N_TP * QW // wide))
        lax.fori_loop(first, stop, weight_grads, 0)

        @pl.when(k == 1)
        def _():
            pass_on(z)

        @pl.when((k >= 3) & (k <= NZ + 1))
        def _():
            pass_on(source(k - 2))

        @pl.when(k == 2)
        def _():
            home(0, z, True)

        @pl.when((k >= 4) & (k <= NZ + 2))
        def _():
            home(k - 3, source(k - 3), False)

        return carry

    lax.fori_loop(0, NZ + 4, step, 0)
    others = ret.at[:, pl.ds(0, N_SP - 1)]
    arrivals = remote(others, others, b_send, b_recv, (sp, right))
    arrivals.wait_recv()
    loads[2].wait()

    returned = ret[...].reshape(2 * n, QW)
    normed_grad[:, mine] = contract_rows(back[...].reshape(2 * n, TOK), returned).astype(BF)
    top, bottom = pl.ds(0, TOK // 2), pl.ds(TOK // 2, TOK // 2)

    def share(side, piece, cols, recv):
        ref = normed_grad.at[(top, bottom)[piece], cols]
        return remote(ref, ref, s_send, recv, (sp, (right, left)[side]))

    for first in (0, 1):
        for side in (0, 1):
            piece = first if side == 0 else 1 - first
            share(side, piece, mine, s_recv.at[side, piece]).start()
    sources = (from_left, from_right)
    for side in (0, 1):
        share(side, side, sources[side], s_recv.at[side, side]).wait_recv()
        share(side, side, sources[side], s_relay.at[side]).start()
    for side in (0, 1):
        share(side, 1 - side, sources[side], s_recv.at[side, 1 - side]).wait_recv()
    for side in (0, 1):
        share(side, side, far, s_relay.at[side]).wait_recv()

    def resid_block(r, carry):
        block = pl.ds(pl.multiple_of(r * RB, RB), RB)
        x = resid[block].astype(F32)
        scale = inv[block]
        g = normed_grad[block].astype(F32) * gain_ref[...]
        pull = scale * scale * scale * jnp.mean(x * g, axis=-1, keepdims=True)
        resid_grad[block] = (grad[block].astype(F32) + scale * g - x * pull).astype(BF)
        return carry

    lax.fori_loop(0, TOK // RB, resid_block, 0)
    pair = sp // 2
    twin = sp + 1 - 2 * core
    chunk = 512
    for c in range(N_TP * QW // chunk):
        term = contract_rows(resid_grad[:, c * chunk : (c + 1) * chunk], conv_out[...])
        pbuf[c * 8 : (c + 1) * 8] = term.reshape(8, 2, 32, CB).astype(BF)
    swap = remote(pbuf.at[:, 1 - core], pswap, p_send, p_recv, (twin, tp))
    swap.start()
    out_grad = jnp.dot(resid_grad[...], proj_w[...], preferred_element_type=F32)
    n_grad = out_grad * dact[...]
    grouped = chan[...]
    sum_grad = inv_std[...] * (
        n_grad
        - jnp.mean(n_grad, axis=-1, keepdims=True)
        - grouped * jnp.mean(n_grad * grouped, axis=-1, keepdims=True)
    )
    ext[pl.ds(0, TOK)] = sum_grad
    last = sp == N_SP - 1
    halo = remote(
        ext.at[pl.ds(0, HALO)], ext.at[pl.ds(TOK, HALO)], h_send, h_recv, (lax.rem(sp + N_SP - 1, N_SP), tp)
    )
    halo.start()
    swap.wait_recv()
    pstage[...] = (pbuf[:, core].astype(F32) + pswap[...].astype(F32)).astype(BF)

    def to_pair(i, carry):
        other = lax.rem(pair + i, N_SP // 2)
        remote(pstage.at[other], precv.at[pair], q_send, q_recv, (2 * other + core, tp)).start()
        return carry

    lax.fori_loop(1, N_SP // 2, to_pair, 0)
    precv[pair] = pstage[pair]

    def finish(first, count):
        total = taps_ref[CONV_K - 1 : CONV_K] * ext[first : first + count]
        for i in range(1, CONV_K):
            total = total + taps_ref[CONV_K - 1 - i : CONV_K - i] * ext[first + i : first + i + count]
        span = slice(first, first + count)
        sigma = jax.nn.sigmoid(cgate_ref[span].astype(F32))
        value_out[span] = (total * sigma).astype(BF)
        gatein_out[span] = (total * cval_ref[span].astype(F32) * sigma * (1.0 - sigma)).astype(BF)

    for block in range(TOK // HALO - 1):
        finish(block * HALO, HALO)
    halo.wait_recv()

    @pl.when(last)
    def _():
        ext[pl.ds(TOK, HALO)] = jnp.zeros((HALO, CB), F32)

    finish(TOK - HALO, HALO)
    others = precv.at[pl.ds(0, N_SP // 2 - 1)]
    remote(others, others, q_send, q_recv, (sp, right)).wait_recv()
    proj_out[...] = jnp.sum(precv[...].astype(F32), axis=0)

    remote(others, others, q_send, q_recv, (sp, right)).wait_send()
    swap.wait_send()
    halo.wait_send()
    share(0, 0, mine, s_recv.at[0, 0]).wait_send()
    share(0, 0, mine, s_recv.at[0, 0]).wait_send()
    share(0, 0, mine, s_recv.at[0, 0]).wait_send()
    share(0, 0, mine, s_recv.at[0, 0]).wait_send()
    share(0, 0, mine, s_recv.at[0, 0]).wait_send()
    share(0, 0, mine, s_recv.at[0, 0]).wait_send()
    arrivals.wait_send()

    def drain(zs, carry):
        for side in (0, 1):
            opposite(side, zs).wait_send()
            onward(side, zs).wait_send()
        return carry

    lax.fori_loop(0, NZ, drain, 0)
    block = group(0, mine)
    for _ in range(3 * NARROW):
        remote(block, block, x_send, x_recv.at[0, 0], (sp, right)).wait_send()
    sent = narrow_send.at[pl.ds(0, NARROW * PER_Z)]
    remote(sent, sent, a_send, a_recv.at[0], (sp, right)).wait_send()
    sent = wide_send.at[pl.ds(0, len(WIDE) * PER_Z - 1)]
    remote(sent, sent, w_send, a_recv.at[0], (sp, right)).wait_send()


def run_experts(
    routes, route_weights, w_gate, w_up, w_down, resid, grad_out, proj, gain, csum, cgain, taps, cval, cgate
):
    width = N_TP * QW
    any_spec = pl.BlockSpec(memory_space=pl.ANY)
    vmem_spec = pl.BlockSpec(memory_space=pltpu.VMEM)
    return pl.pallas_call(
        experts_kernel,
        out_shape=(
            pltpu.VMEM((width, FH), BF),
            pltpu.VMEM((width, FH), BF),
            pltpu.VMEM((FH, width), BF),
            pltpu.VMEM((32, CB), F32),
            pltpu.VMEM((TOK, CB), BF),
            pltpu.VMEM((TOK, CB), BF),
        ),
        in_specs=[vmem_spec] * 2 + [any_spec] * 6 + [vmem_spec] * 6,
        out_specs=(vmem_spec,) * 6,
        scratch_shapes=[
            pltpu.VMEM((2, N_SP, 8, QW), BF),
            pltpu.VMEM((3, N_SP, 8, width), BF),
            pltpu.VMEM((width, FH), BF),
            pltpu.VMEM((width, FH), BF),
            pltpu.VMEM((FH, width), BF),
            pltpu.VMEM((2, N_SP, 8, FH), BF),
            pltpu.VMEM((2, N_SP, 8, FH), BF),
            pltpu.VMEM((2, N_SP, 8, FH), BF),
            pltpu.VMEM((NZ, TILES, 8, width), BF),
            pltpu.VMEM((2, NZ, HALF, 8, QW), BF),
            pltpu.VMEM((2, NZ, TILES, 8, QW), BF),
            pltpu.VMEM((2, NZ, TILES, 8, QW), BF),
            pltpu.VMEM((NZ, TILES, 8, QW), BF),
            pltpu.VMEM((TOK, width), BF),
            pltpu.VMEM((TOK, width), BF),
            pltpu.VMEM((TOK, width), BF),
            pltpu.VMEM((NZ, 2 * PER_Z * 8, TOK), BF),
            pltpu.VMEM((2, NZ, PER_Z * 8, TOK), BF),
            pltpu.VMEM((NZ, 2 * PER_Z * 8, 1), F32),
            pltpu.VMEM((len(WIDE) * PER_Z, 3, 8, width), BF),
            pltpu.VMEM((NARROW * PER_Z, 3, 8, QW), BF),
            pltpu.VMEM((width, CB), BF),
            pltpu.VMEM((TOK, 1), F32),
            pltpu.VMEM((TOK, CB), F32),
            pltpu.VMEM((TOK, 1), F32),
            pltpu.VMEM((TOK, CB), F32),
            pltpu.VMEM((TOK, CB), BF),
            pltpu.VMEM((TOK, width), BF),
            pltpu.VMEM((TOK, width), BF),
            pltpu.VMEM((N_SP // 2, 2, 32, CB), BF),
            pltpu.VMEM((N_SP // 2, 32, CB), BF),
            pltpu.VMEM((N_SP // 2, 32, CB), BF),
            pltpu.VMEM((N_SP // 2, 32, CB), BF),
            pltpu.VMEM((TOK + HALO, CB), F32),
            pltpu.SemaphoreType.DMA((3,)),
            pltpu.SemaphoreType.DMA,
            pltpu.SemaphoreType.DMA((2, 2)),
            pltpu.SemaphoreType.DMA((2,)),
            pltpu.SemaphoreType.DMA,
            pltpu.SemaphoreType.DMA,
            pltpu.SemaphoreType.DMA,
            pltpu.SemaphoreType.DMA,
            pltpu.SemaphoreType.DMA,
            pltpu.SemaphoreType.DMA,
            pltpu.SemaphoreType.DMA,
            pltpu.SemaphoreType.DMA,
            pltpu.SemaphoreType.DMA((NZ,)),
            pltpu.SemaphoreType.DMA,
            pltpu.SemaphoreType.DMA((2, NZ)),
            pltpu.SemaphoreType.DMA((2, NZ)),
            pltpu.SemaphoreType.DMA((3,)),
            pltpu.SemaphoreType.DMA,
            pltpu.SemaphoreType.DMA((2, NZ)),
            pltpu.SemaphoreType.DMA,
            pltpu.SemaphoreType.DMA((2, NZ)),
            pltpu.SemaphoreType.DMA,
            pltpu.SemaphoreType.DMA,
        ],
        compiler_params=pltpu.CompilerParams(collective_id=0, has_side_effects=True, vmem_limit_bytes=48 << 20),
        name="experts",
    )(
        routes, route_weights, w_gate, w_up, w_down, resid, grad_out, proj, gain, csum, cgain, taps, cval, cgate
    )


def contract_rows(left_side, right_side):
    return lax.dot_general(
        left_side, right_side, (((0,), (0,)), ((), ())), preferred_element_type=jnp.float32
    )


def contract_cols(left_side, right_side):
    return lax.dot_general(
        left_side, right_side, (((1,), (1,)), ((), ())), preferred_element_type=jnp.float32
    )


def local(
    grad_out,
    resid,
    norm_gain,
    routes,
    route_weights,
    gate_weight,
    up_weight,
    down_weight,
    proj_weight,
    conv_sum,
    conv_gain,
    conv_taps,
    conv_value,
    conv_gate,
):
    gate_grad, up_grad, down_grad, proj_grad, value_grad, gate_input_grad = run_experts(
        routes.T,
        route_weights.T,
        gate_weight[0],
        up_weight[0],
        down_weight[0],
        resid,
        grad_out,
        proj_weight,
        norm_gain[None],
        conv_sum,
        conv_gain[None],
        conv_taps,
        conv_value,
        conv_gate,
    )
    return (gate_grad[None], up_grad[None], down_grad[None], proj_grad, value_grad, gate_input_grad)


def solution(mesh):
    in_specs = (
        P("sp", None),
        P("sp", None),
        P(),
        P("sp", None),
        P("sp", None),
        P("sp", None, "tp"),
        P("sp", None, "tp"),
        P("sp", "tp", None),
        P(None, "tp"),
        P("sp", "tp"),
        P("tp"),
        P(None, "tp"),
        P("sp", "tp"),
        P("sp", "tp"),
    )
    out_specs = (
        P("sp", None, "tp"),
        P("sp", None, "tp"),
        P("sp", "tp", None),
        P("sp", "tp"),
        P("sp", "tp"),
        P("sp", "tp"),
    )
    return jax.shard_map(local, mesh=mesh, in_specs=in_specs, out_specs=out_specs, check_vma=False)
```
